256 devices in a mesh: rep: 64 (over z, y, core), fs: 2 (over x_lo), tp: 2 (over x_hi).
Axes of the slice: x: 4 (x_hi: 2, x_lo: 2; x = x_hi * 2 + x_lo), y: 4, z: 8, core: 2. Of those that a mesh axis runs over, the one named last changes fastest.
Arguments:
- inputs: bfloat16 [32768, 2048], P(('rep', 'tp'), 'fs'), may hold values from -6 to 6
- pre_act: bfloat16 [32768, 4096], P(('rep', 'fs'), 'tp'), may hold values from -6 to 6
- cotangent: bfloat16 [32768, 2048], P(('rep', 'tp'), 'fs'), may hold values from -24 to 24
- up_weight: bfloat16 [2048, 4096], P('fs', 'tp'), may hold values from -0.125 to 0.125
- down_weight: bfloat16 [4096, 2048], P('tp', 'fs'), may hold values from -0.09375 to 0.09375
Outputs:
- grad_inputs: bfloat16 [32768, 2048], P(('rep', 'tp'), 'fs')
- grad_up: float32 [2048, 4096], P('fs', 'tp')
- grad_down: float32 [4096, 2048], P('tp', 'fs')
The draws below stay inside these ranges and needn't reach their ends.
All inputs are finite; a program needn't handle non-finite values.
Results may differ from the reference program's by a relative error of at most 0.015.
Values may be sent and summed in bfloat16 or wider, within the bound.
No kernel may reach another device: no remote copies, remote signals or barrier semaphores. Data moves between devices by JAX's collectives and lax.ppermute only.
A program may use at most 128 MiB of HBM per device.

```python
import jax
import jax.numpy as jnp
from jax import lax

D = 2048
FF = 4096
TOKENS = 32768
N_TP = 2


def raised(array, rng, source, target, parts, factor):
    owner, partner = [(jnp.arange(array.shape[position]) // (array.shape[position] // parts)).reshape([-1 if axis == position else 1 for axis in range(array.ndim)]) for position in (source, target)]
    chosen = jax.random.permutation(rng, parts)[partner]
    strong = (owner == chosen) | (owner == (partner + parts // 2) % parts)
    return jnp.where(strong, factor * array, array)


def block_levels(stream_key, shape, shards, low, top_value):
    def one(dim, blocks):
        heights = jax.random.uniform(jax.random.fold_in(jax.random.fold_in(stream_key, 6), dim), (blocks,), jnp.float32, low / len(shards), top_value / len(shards))
        return jnp.repeat(jnp.exp(heights), shape[dim] // blocks).reshape((-1,) + (1,) * (len(shape) - dim - 1))

    level = one(*shards[0])
    for cut in shards[1:]:
        level = level * one(*cut)
    return level


def bell_draw(key, dims, scale, reach, pieces=(), held_as=jnp.bfloat16):
    values = jax.random.normal(key, dims, jnp.float32) * scale
    if len(pieces) > 0:
        values = block_levels(key, dims, pieces, -0.22, 0.18) * values
    return jnp.clip(values, min=-reach, max=reach).astype(held_as)


def bell_draw_with(rng, shape, spread, limit, split, heavy, dtype=jnp.bfloat16):
    entries = spread * jax.random.normal(rng, shape, jnp.float32)
    if split:
        entries = entries * block_levels(rng, shape, split, -0.22, 0.18)
    return jnp.clip(raised(entries, jax.random.fold_in(rng, 3), *heavy), -limit, limit).astype(dtype)


def setup_inputs(seed: int = 0) -> dict:
    splits = jax.random.split(jax.random.key(seed), 6)
    return {
        "inputs": bell_draw(splits[0], (TOKENS, D), 1.0, 6.0, ((0, 128), (1, 2))),
        "pre_act": bell_draw(splits[1], (TOKENS, FF), 1.0, 6.0, ((0, 128), (1, 2))),
        "cotangent": bell_draw_with(splits[2], (TOKENS, D), 1.0, 24.0, ((0, 128), (1, 2)), (0, 1, 128, 5.5)),
        "up_weight": bell_draw(splits[3], (D, FF), D ** -0.5, 0.125, ((0, 2), (1, 2))),
        "down_weight": bell_draw(splits[4], (FF, D), FF ** -0.5, 0.09375, ((0, 2), (1, 2))),
    }


def reference(inputs, pre_act, cotangent, up_weight, down_weight):
    positive = jnp.maximum(pre_act.astype(jnp.float32), 0.0)
    square = (positive * positive).astype(jnp.bfloat16)
    grad_act = jnp.dot(cotangent, down_weight.T, preferred_element_type=jnp.float32)
    grad_pre = (2.0 * positive * grad_act).astype(jnp.bfloat16)
    factor = TOKENS ** -0.5
    grad_down = jnp.dot(square.T, cotangent, preferred_element_type=jnp.float32) * factor
    grad_up = jnp.dot(inputs.T, grad_pre, preferred_element_type=jnp.float32) * factor
    width = FF // N_TP
    total = jnp.zeros(inputs.shape, jnp.float32)
    for block in range(N_TP):
        partial_sum = jnp.dot(grad_pre[:, block * width:(block + 1) * width],
                              up_weight[:, block * width:(block + 1) * width].T,
                              preferred_element_type=jnp.float32).astype(jnp.bfloat16)
        partial_sum = lax.optimization_barrier(partial_sum)
        total = total + partial_sum.astype(jnp.float32)
    grad_inputs = total.astype(jnp.bfloat16)
    return grad_inputs, grad_up, grad_down
```

```python
import jax
import jax.numpy as jnp
from jax import lax
from jax.sharding import PartitionSpec as P


NY = 4
NC = 2
AXES = ("rep", "fs", "tp")


class Place:
    def __init__(self):
        self.reps = lax.axis_size("rep")
        self.nz = self.reps // (NY * NC)
        rep = lax.axis_index("rep")
        self.c = rep % NC
        self.fs = lax.axis_index("fs")
        self.tp = lax.axis_index("tp")

    def send(self, value, dz=0, y=0, c=0, fs=0, tp=0):
        pairs = []
        for r in range(self.reps):
            z0, y0, c0 = r // (NY * NC), r // NC % NY, r % NC
            target = (((z0 + dz) % self.nz) * NY + (y0 ^ y)) * NC + (c0 ^ c)
            for f in range(2):
                for t in range(2):
                    pairs.append(((r * 2 + f) * 2 + t, (target * 2 + (f ^ fs)) * 2 + (t ^ tp)))
        return lax.ppermute(value, AXES, pairs)

    def y_groups(self):
        return [[(z * NY + y) * NC + c for y in range(NY)] for z in range(self.nz) for c in range(NC)]

    def z_groups(self):
        return [[(z * NY + y) * NC + c for z in range(self.nz)] for y in range(NY) for c in range(NC)]


def exchange(value, groups):
    return lax.all_to_all(value, "rep", 0, 0, axis_index_groups=groups, tiled=True)


def to_all(value, groups):
    return exchange(jnp.broadcast_to(value[None], (len(groups[0]), *value.shape)), groups)


def added(*values):
    total = values[0].astype(jnp.float32)
    for value in values[1:]:
        total = total + value.astype(jnp.float32)
    return total.astype(jnp.bfloat16)


def rows_of(value, start, size):
    return lax.dynamic_slice_in_dim(value, start, size, axis=0)


def cols_of(value, start, size):
    return lax.dynamic_slice_in_dim(value, start, size, axis=1)


def ordered(flag, own, other):
    return jnp.where(flag, other, own), jnp.where(flag, own, other)


def ring_gather(me, block):
    half = block.shape[0] // 2
    near = me.send(block, fs=1)
    diag = me.send(block, fs=1, tp=1)
    first = me.send(near[:half], fs=1, tp=1)
    second = me.send(diag[half:], fs=1)
    return block, near, jnp.concatenate([first, second]), diag


def ring_sum(me, own, near, far, diag):
    half = own.shape[0] // 2
    a1 = me.send(far[:half], fs=1)
    b1 = me.send(far[half:], fs=1, tp=1)
    a2 = me.send(near[:half], fs=1)
    b2 = me.send(diag[half:], fs=1, tp=1)
    a3 = me.send(added(diag[:half], a1), fs=1, tp=1)
    b3 = me.send(added(near[half:], b1), fs=1)
    return jnp.concatenate([added(own[:half], a2, a3), added(own[half:], b2, b3)])


def contract_rows(left, right):
    return lax.dot_general(left, right, (((0,), (0,)), ((), ())), preferred_element_type=jnp.float32)


def contract_cols(left, right):
    return lax.dot_general(left, right, (((1,), (1,)), ((), ())), preferred_element_type=jnp.float32)


def tokens_of(blocks):
    own, near, far, diag = blocks
    return jnp.concatenate([jnp.concatenate([own, near], 1), jnp.concatenate([far, diag], 1)], 0)


def per_device(inputs, pre_act, cotangent, up_weight, down_weight):
    me = Place()
    nz = me.nz
    width = pre_act.shape[1]
    quarter, eighth = width // 2, width // 4
    half_d = inputs.shape[1]
    factor = (inputs.shape[0] * me.reps * lax.axis_size("tp")) ** (-0.5)
    mine, theirs = me.fs * quarter, (1 - me.fs) * quarter
    first, second = me.c * eighth, (1 - me.c) * eighth

    cot = tokens_of(ring_gather(me, cotangent))
    pre_near = me.send(cols_of(pre_act, theirs, quarter), fs=1)
    pre_own = cols_of(pre_act, mine, quarter)
    pre = jnp.concatenate(ordered(me.fs != me.tp, pre_own, pre_near), 0)

    down_near = me.send(rows_of(down_weight, theirs + first, eighth), fs=1)
    down_other = me.send(down_near, c=1)
    x = tokens_of(ring_gather(me, inputs))
    up_near = me.send(cols_of(up_weight, theirs + first, eighth), fs=1)
    up_other = me.send(up_near, c=1)

    down = (
        jnp.concatenate([rows_of(down_weight, mine + first, eighth), down_near], 1),
        jnp.concatenate([rows_of(down_weight, mine + second, eighth), down_other], 1),
    )
    up = (
        jnp.concatenate([cols_of(up_weight, mine + first, eighth), up_near], 0),
        jnp.concatenate([cols_of(up_weight, mine + second, eighth), up_other], 0),
    )
    positive = tuple(
        jnp.maximum(cols_of(pre, start, eighth).astype(jnp.float32), 0.0) for start in (first, second)
    )
    square = tuple((p * p).astype(jnp.bfloat16) for p in positive)

    down_parts = tuple(contract_rows(s, cot).astype(jnp.bfloat16) for s in square)
    grad_pre = tuple(
        (2.0 * p * contract_cols(cot, w)).astype(jnp.bfloat16) for p, w in zip(positive, down)
    )
    up_parts = tuple(contract_rows(x, g).astype(jnp.bfloat16) for g in grad_pre)

    rows_down = eighth // (NY * nz)
    down_sum = added(down_parts[0], me.send(down_parts[1], c=1))
    down_sum = down_sum.reshape(NY, nz, rows_down, 2 * half_d)
    rows_up = half_d // (NY * nz)
    up_sum = added(up_parts[0], me.send(up_parts[1], c=1))
    up_sum = up_sum.reshape(2, NY, nz, rows_up, eighth).transpose(1, 2, 0, 3, 4)

    def scattered(value):
        got = exchange(value, me.y_groups())
        got = added(*[got[i] for i in range(NY)])
        got = exchange(got, me.z_groups())
        return added(*[got[i] for i in range(nz)])

    def everywhere(value):
        got = to_all(value, me.z_groups()).reshape(nz, *value.shape)
        got = to_all(got, me.y_groups()).reshape(NY, nz, *value.shape)
        return jnp.stack(ordered(me.c == 1, got, me.send(got, c=1)))

    d = scattered(down_sum)
    d = jnp.stack(ordered(me.fs == 1, d[:, :half_d], me.send(d[:, half_d:], fs=1)))
    d = everywhere(d)
    grad_down = (d.astype(jnp.float32) * factor).transpose(3, 0, 1, 2, 4, 5).reshape(width, half_d)

    u = scattered(up_sum)
    u = jnp.stack(ordered(me.fs == 1, u[0], me.send(u[1], fs=1)))
    u = everywhere(u)
    grad_up = (u.astype(jnp.float32) * factor).transpose(1, 2, 4, 3, 0, 5).reshape(half_d, width)

    part = (contract_cols(grad_pre[0], up[0]) + contract_cols(grad_pre[1], up[1])).astype(jnp.bfloat16)
    rows = inputs.shape[0]
    grad_inputs = ring_sum(
        me,
        part[:rows, :half_d],
        part[:rows, half_d:],
        part[rows:, :half_d],
        part[rows:, half_d:],
    )
    return grad_inputs, grad_up, grad_down


def solution(mesh):
    tokens = P(("rep", "tp"), "fs")
    return jax.shard_map(
        per_device,
        mesh=mesh,
        in_specs=(tokens, P(("rep", "fs"), "tp"), tokens, P("fs", "tp"), P("tp", "fs")),
        out_specs=(tokens, P("fs", "tp"), P("tp", "fs")),
        check_vma=False,
    )
```

```python
import jax
import jax.numpy as jnp
from jax import lax
from jax.experimental import pallas as pl
from jax.experimental.pallas import tpu as pltpu
from jax.sharding import Mesh
from jax.sharding import PartitionSpec as P


NY = 4
NC = 2
AXES = ("z", "y", "c", "fs", "tp")
REP = ("z", "y", "c")


def send(value, y=0, c=0, fs=0, tp=0):
    sizes = [lax.axis_size(axis) for axis in AXES]
    flips = (0, y, c, fs, tp)
    pairs = []
    total = 1
    for size in sizes:
        total *= size
    for source in range(total):
        rest, at = source, []
        for size in reversed(sizes):
            at.append(rest % size)
            rest //= size
        target = 0
        for size, place, flip in zip(sizes, reversed(at), flips):
            target = target * size + (place ^ flip)
        pairs.append((source, target))
    return lax.ppermute(value, AXES, pairs)


def exchange(value, axes):
    shape = value.shape
    flat = value.reshape(-1, *shape[2:]) if isinstance(axes, tuple) else value
    return lax.all_to_all(flat, axes, 0, 0, tiled=True).reshape(shape)


def to_all(value, axis):
    peers = lax.axis_size(axis)
    return exchange(jnp.broadcast_to(value[None], (peers, *value.shape)), axis)


def added(*values):
    total = values[0].astype(jnp.float32)
    for value in values[1:]:
        total = total + value.astype(jnp.float32)
    return total.astype(jnp.bfloat16)


def rows_of(value, start, size):
    return lax.dynamic_slice_in_dim(value, start, size, axis=0)


def cols_of(value, start, size):
    return lax.dynamic_slice_in_dim(value, start, size, axis=1)


def ordered(flag, own, other):
    return jnp.where(flag, other, own), jnp.where(flag, own, other)


def ring_sum(own, near, far, diag):
    half = own.shape[0] // 2
    a1 = send(jnp.concatenate([far[:half], near[:half]]), fs=1)
    b1 = send(jnp.concatenate([far[half:], diag[half:]]), fs=1, tp=1)
    a2 = send(added(diag[:half], a1[:half]), fs=1, tp=1)
    b2 = send(added(near[half:], b1[:half]), fs=1)
    return jnp.concatenate([added(own[:half], a1[half:], a2), added(own[half:], b1[half:], b2)])


def contract_rows(left, right):
    return lax.dot_general(left, right, (((0,), (0,)), ((), ())), preferred_element_type=jnp.float32)


def contract_cols(left, right):
    return lax.dot_general(left, right, (((1,), (1,)), ((), ())), preferred_element_type=jnp.float32)


def tokens_of(own, near, far, diag):
    return jnp.concatenate([jnp.concatenate([own, near], 1), jnp.concatenate([far, diag], 1)], 0)


def laid(out, pieces, shape, place, scale):
    nz, nf, rows, columns = pieces[0][2].shape
    count = len(pieces)
    at = jnp.stack([part for y, c, _ in pieces for part in (y, c)]).astype(jnp.int32)

    def kernel(at, *refs):
        for index in range(count):
            for f in range(nf):

                @pl.when((pl.program_id(0) == index) & (pl.program_id(1) == f))
                def _(source=refs[index], target=refs[-1], f=f):
                    target[...] = source[:, f].reshape(nz * rows, columns).astype(jnp.float32) * scale

    arguments = (at, *[value for _, _, value in pieces]) + (() if out is None else (out,))
    specs = [pl.BlockSpec((nz, nf, rows, columns), lambda i, f, at: (0, 0, 0, 0)) for _ in pieces]
    specs += [] if out is None else [pl.BlockSpec(memory_space=pl.ANY)]
    return pl.pallas_call(
        kernel,
        grid_spec=pltpu.PrefetchScalarGridSpec(
            num_scalar_prefetch=1,
            grid=(count, nf),
            in_specs=specs,
            out_specs=pl.BlockSpec(
                (nz * rows, columns), lambda i, f, at: place(f, at[2 * i], at[2 * i + 1])
            ),
        ),
        out_shape=jax.ShapeDtypeStruct(shape, jnp.float32),
        input_output_aliases={} if out is None else {count + 1: 0},
        cost_estimate=pl.CostEstimate(
            flops=count * pieces[0][2].size,
            bytes_accessed=count * pieces[0][2].size * 6,
            transcendentals=0,
        ),
    )(*arguments)


def per_device(inputs, pre_act, cotangent, up_weight, down_weight):
    nz = lax.axis_size("z")
    _, y, c, fs, tp = (lax.axis_index(axis) for axis in AXES)
    width = pre_act.shape[1]
    quarter, eighth = width // 2, width // 4
    half_d = inputs.shape[1]
    rows = inputs.shape[0]
    factor = (rows * nz * NY * NC * 2) ** (-0.5)
    mine, theirs = fs * quarter, (1 - fs) * quarter
    first, second = c * eighth, (1 - c) * eighth
    rows_down, rows_up = eighth // (NY * nz), half_d // (NY * nz)

    down_near = send(rows_of(down_weight, theirs + first + y * (eighth // NY), eighth // NY), fs=1)
    cot_near = send(cotangent, fs=1)
    cot_diag = send(cotangent, fs=1, tp=1)
    pre_near = send(cols_of(pre_act, theirs, quarter), fs=1)
    down_near = to_all(down_near, "y").reshape(eighth, half_d)
    down_other = send(down_near, c=1)
    cot_far = send(cot_near, fs=1, tp=1)
    in_near = send(inputs, fs=1)
    in_diag = send(inputs, fs=1, tp=1)
    in_far = send(in_near, fs=1, tp=1)
    up_near = send(cols_of(up_weight, theirs + first, eighth), fs=1)
    up_other = send(up_near, c=1)

    cot = lax.optimization_barrier(tokens_of(cotangent, cot_near, cot_far, cot_diag))
    pre_own = cols_of(pre_act, mine, quarter)
    pre = jnp.concatenate(ordered(fs != tp, pre_own, pre_near), 0)
    positive = tuple(
        jnp.maximum(cols_of(pre, start, eighth).astype(jnp.float32), 0.0) for start in (first, second)
    )
    square = lax.optimization_barrier(tuple((p * p).astype(jnp.bfloat16) for p in positive))

    down_parts = tuple(contract_rows(s, cot).astype(jnp.bfloat16) for s in square)
    down_parts = (down_parts[0], send(down_parts[1], c=1))

    down = (
        lax.optimization_barrier(jnp.concatenate([rows_of(down_weight, mine + first, eighth), down_near], 1)),
        lax.optimization_barrier(jnp.concatenate([rows_of(down_weight, mine + second, eighth), down_other], 1)),
    )
    grad_pre = tuple(
        (2.0 * p * contract_cols(cot, w)).astype(jnp.bfloat16) for p, w in zip(positive, down)
    )
    x = lax.optimization_barrier(tokens_of(inputs, in_near, in_far, in_diag))
    up_parts = tuple(contract_rows(x, g).astype(jnp.bfloat16) for g in grad_pre)
    up_parts = (up_parts[0], send(up_parts[1], c=1))

    def down_chunk(flip, half):
        size = eighth // NY // 2
        return [rows_of(part, (y ^ flip) * 2 * size + half * size, size) for part in down_parts]

    def up_chunk(flip, half):
        size = half_d // NY
        return [rows_of(part, half * half_d + (y ^ flip) * size, size) for part in up_parts]

    def y_sum(chunk):
        one = jnp.stack([added(*chunk(2, 0)), added(*chunk(1, 0))])
        three = jnp.stack([added(*chunk(2, 1)), added(*chunk(3, 1))])
        rest = [added(*chunk(*which)) for which in ((1, 1), (3, 0), (0, 0), (0, 1))]
        one, three, to_one, to_three, first, second = lax.optimization_barrier((one, three, *rest))
        one = send(one, y=1)
        three = send(three, y=3)
        right = send(added(to_one, three[0]), y=1)
        left = send(added(to_three, one[0]), y=3)
        return added(first, one[1], left), added(second, three[1], right)

    def z_sum(value):
        got = exchange(value, "z")
        return added(*[got[i] for i in range(nz)])

    def gathered(own, other):
        both = jnp.stack(ordered(fs == 1, own, other))
        both = jnp.broadcast_to(both[None], (nz, *both.shape))
        value = exchange(both, ("z", "fs"))
        one, three = send(value, y=1), send(value, y=3)
        half = nz // 2
        two = jnp.concatenate([send(one[:half], y=3), send(three[half:], y=1)])
        near, far = [(y, value), (y ^ 1, one), (y ^ 3, three)], [(y ^ 2, two)]
        return [[(p, c, v) for p, v in group] + [(p, 1 - c, send(v, c=1)) for p, v in group] for group in (near, far)]

    d = jnp.concatenate(y_sum(down_chunk)).reshape(nz, rows_down, 2 * half_d)
    d = z_sum(d)
    u = jnp.stack([half.reshape(nz, rows_up, eighth) for half in y_sum(up_chunk)], 1)
    u = z_sum(u)
    place_down = lambda f, y, c: (f * (NC * NY) + c * NY + y, 0)
    place_up = lambda f, y, c: (y, f * NC + c)
    near, far = gathered(d[:, :half_d], d[:, half_d:])
    grad_down = laid(None, near, (width, half_d), place_down, factor)
    grad_down = laid(grad_down, far, (width, half_d), place_down, factor)
    near, far = gathered(u[0], u[1])
    grad_up = laid(None, near, (half_d, width), place_up, factor)
    grad_up = laid(grad_up, far, (half_d, width), place_up, factor)

    up = (
        jnp.concatenate([cols_of(up_weight, mine + first, eighth), up_near], 0),
        jnp.concatenate([cols_of(up_weight, mine + second, eighth), up_other], 0),
    )
    part = (contract_cols(grad_pre[0], up[0]) + contract_cols(grad_pre[1], up[1])).astype(jnp.bfloat16)
    grad_inputs = ring_sum(
        part[:rows, :half_d],
        part[:rows, half_d:],
        part[rows:, :half_d],
        part[rows:, half_d:],
    )
    return grad_inputs, grad_up, grad_down


def solution(mesh):
    reps = mesh.shape["rep"]
    split = Mesh(mesh.devices.reshape(reps // (NY * NC), NY, NC, 2, 2), AXES)
    tokens = P((*REP, "tp"), "fs")

    return jax.shard_map(
        per_device,
        mesh=split,
        in_specs=(tokens, P((*REP, "fs"), "tp"), tokens, P("fs", "tp"), P("tp", "fs")),
        out_specs=(tokens, P("fs", "tp"), P("tp", "fs")),
        check_vma=False,
    )
```

```python
import jax
import jax.numpy as jnp
from jax import lax
from jax.experimental import pallas as pl
from jax.experimental.pallas import tpu as pltpu
from jax.sharding import Mesh
from jax.sharding import PartitionSpec as P


NY = 4
NC = 2
AXES = ("z", "y", "c", "fs", "tp")
REP = ("z", "y", "c")


def send(value, y=0, c=0, fs=0, tp=0):
    sizes = [lax.axis_size(axis) for axis in AXES]
    flips = (0, y, c, fs, tp)
    pairs = []
    total = 1
    for size in sizes:
        total *= size
    for source in range(total):
        rest, at = source, []
        for size in reversed(sizes):
            at.append(rest % size)
            rest //= size
        target = 0
        for size, place, flip in zip(sizes, reversed(at), flips):
            target = target * size + (place ^ flip)
        pairs.append((source, target))
    return lax.ppermute(value, AXES, pairs)


def exchange(value, axis):
    return lax.all_to_all(value, axis, 0, 0, tiled=True)


def to_all(value, axis):
    peers = lax.axis_size(axis)
    return exchange(jnp.broadcast_to(value[None], (peers, *value.shape)), axis)


def added(*values):
    total = values[0].astype(jnp.float32)
    for value in values[1:]:
        total = total + value.astype(jnp.float32)
    return total.astype(jnp.bfloat16)


def rows_of(value, start, size):
    return lax.dynamic_slice_in_dim(value, start, size, axis=0)


def cols_of(value, start, size):
    return lax.dynamic_slice_in_dim(value, start, size, axis=1)


def ordered(flag, own, other):
    return jnp.where(flag, other, own), jnp.where(flag, own, other)


def ring_sum(own, near, far, diag):
    return added(own, send(near, fs=1), send(diag, fs=1, tp=1), send(far, tp=1))


def contract_rows(left, right):
    return lax.dot_general(left, right, (((0,), (0,)), ((), ())), preferred_element_type=jnp.float32)


def contract_cols(left, right):
    return lax.dot_general(left, right, (((1,), (1,)), ((), ())), preferred_element_type=jnp.float32)


def tokens_of(own, near, far, diag):
    return jnp.concatenate([jnp.concatenate([own, near], 1), jnp.concatenate([far, diag], 1)], 0)


CHUNKS = ((2, 0), (1, 0), (2, 1), (3, 1), (1, 1), (3, 0), (0, 0), (0, 1))


def chunk_sums(y, own, partner, halves_first):
    rows, columns = own.shape[2:]
    at = jnp.stack([part for flip, half in CHUNKS for part in (y ^ flip, half)]).astype(jnp.int32)

    def kernel(at, own, partner, one, three, rest):
        total = (own[0].astype(jnp.float32) + partner[0].astype(jnp.float32)).astype(jnp.bfloat16)
        step = pl.program_id(0)
        for target, low, high in ((one, 0, 2), (three, 2, 4), (rest, 4, 8)):

            @pl.when((step >= low) & (step < high))
            def _(target=target):
                target[...] = total

    def source(i, at):
        return (at[2 * i + 1], at[2 * i], 0, 0) if halves_first else (at[2 * i], at[2 * i + 1], 0, 0)

    def target(low, high):
        return pl.BlockSpec((1, rows, columns), lambda i, at: (jnp.clip(i - low, 0, high - low - 1), 0, 0))

    return pl.pallas_call(
        kernel,
        grid_spec=pltpu.PrefetchScalarGridSpec(
            num_scalar_prefetch=1,
            grid=(len(CHUNKS),),
            in_specs=[pl.BlockSpec((1, 1, rows, columns), source)] * 2,
            out_specs=[target(0, 2), target(2, 4), target(4, 8)],
        ),
        out_shape=[jax.ShapeDtypeStruct((n, rows, columns), jnp.bfloat16) for n in (2, 2, 4)],
        cost_estimate=pl.CostEstimate(flops=own.size, bytes_accessed=own.size * 6, transcendentals=0),
    )(at, own, partner)


def laid(out, group, c, shape, by_rows, scale):
    places, own, partner = group
    count, nz, nf, rows, columns = partner.shape
    at = jnp.concatenate([places, c[None]]).astype(jnp.int32)

    def kernel(at, *refs):
        target = refs[-1]

        def put(source, core):
            def step(i, _):
                z, f = i // nf, i % nf
                wide = source[z, f].astype(jnp.float32) * scale
                lines = pl.ds(pl.multiple_of(z * rows, rows), rows)
                if by_rows:
                    target[f, core, 0, lines] = wide
                else:
                    left = pl.multiple_of((f * NC + core) * columns, columns)
                    target[lines, pl.ds(left, columns)] = wide
                return _

            lax.fori_loop(0, nz * nf, step, 0)

        for index in range(count):

            @pl.when(pl.program_id(0) == index)
            def _(source=refs[index]):
                put(source, at[count])

        put(refs[count].at[0], 1 - at[count])

    arguments = (at, *own, partner) + (() if out is None else (out,))
    specs = [pl.BlockSpec((nz, nf, rows, columns), lambda i, at: (0, 0, 0, 0)) for _ in own]
    specs += [pl.BlockSpec((1, nz, nf, rows, columns), lambda i, at: (i, 0, 0, 0, 0))]
    specs += [] if out is None else [pl.BlockSpec(memory_space=pl.ANY)]
    if by_rows:
        out_spec = pl.BlockSpec((nf, NC, 1, nz * rows, columns), lambda i, at: (0, 0, at[i], 0, 0))
    else:
        out_spec = pl.BlockSpec((nz * rows, nf * NC * columns), lambda i, at: (at[i], 0))
    return pl.pallas_call(
        kernel,
        grid_spec=pltpu.PrefetchScalarGridSpec(
            num_scalar_prefetch=1, grid=(count,), in_specs=specs, out_specs=out_spec
        ),
        out_shape=jax.ShapeDtypeStruct(shape, jnp.float32),
        input_output_aliases={} if out is None else {count + 2: 0},
        cost_estimate=pl.CostEstimate(
            flops=2 * partner.size, bytes_accessed=partner.size * 12, transcendentals=0
        ),
    )(*arguments)


def per_device(inputs, pre_act, cotangent, up_weight, down_weight):
    nz = lax.axis_size("z")
    z, y, c, fs, tp = (lax.axis_index(axis) for axis in AXES)
    width = pre_act.shape[1]
    quarter, eighth = width // 2, width // 4
    half_d = inputs.shape[1]
    rows = inputs.shape[0]
    factor = (rows * nz * NY * NC * 2) ** (-0.5)
    mine, theirs = fs * quarter, (1 - fs) * quarter
    first, second = c * eighth, (1 - c) * eighth
    rows_down, rows_up = eighth // (NY * nz), half_d // (NY * nz)
    fixed = lax.optimization_barrier

    def cols_by_core(value, start):
        return jnp.concatenate([cols_of(value, start + first, eighth), cols_of(value, start + second, eighth)], 1)

    down_near = rows_of(down_weight, theirs + first + y * (eighth // NY), eighth // NY)
    cot_near = send(jnp.concatenate([cotangent, down_near]), fs=1)
    cot_near, down_near = fixed((cot_near[:rows], cot_near[rows:]))
    cot_diag = send(cotangent, fs=1, tp=1)
    pre_near = send(cols_by_core(pre_act, theirs), fs=1)
    down_near = to_all(down_near, "y").reshape(eighth, half_d)
    down_other = send(down_near, c=1)
    cot_far = send(cot_near, fs=1, tp=1)
    in_near = send(inputs, fs=1)
    in_diag = send(inputs, fs=1, tp=1)
    in_far = send(inputs, tp=1)
    up_near = send(cols_of(up_weight, theirs + first, eighth), fs=1)
    up_other = send(up_near, c=1)

    down_own = fixed(
        jnp.concatenate(
            [rows_of(down_weight, mine + first, eighth), rows_of(down_weight, mine + second, eighth)]
        )
    )
    cot = fixed(tokens_of(cotangent, cot_near, cot_far, cot_diag))
    pre = jnp.concatenate(ordered(fs != tp, cols_by_core(pre_act, mine), pre_near), 0)
    positive = jnp.maximum(pre.astype(jnp.float32), 0.0)
    square = fixed(
        tuple((p * p).astype(jnp.bfloat16) for p in (positive[:, :eighth], positive[:, eighth:]))
    )
    down_part = contract_rows(square[0], cot).astype(jnp.bfloat16)
    down_parts = (down_part, send(contract_rows(square[1], cot).astype(jnp.bfloat16), c=1))

    split = (NY, 2, eighth // NY // 2, 2 * half_d)
    down_sums = chunk_sums(y, *[part.reshape(split) for part in down_parts], False)

    down = fixed(jnp.concatenate([down_own, fixed(jnp.concatenate([down_near, down_other]))], 1))
    grad_pre = fixed((2.0 * positive * contract_cols(cot, down)).astype(jnp.bfloat16))
    grad_pre, *ready = fixed((grad_pre, inputs, in_near, in_far, in_diag, down_sums[0][0, :1]))[:5]
    x = fixed(tokens_of(*ready))
    up_parts = tuple(
        contract_rows(x, g).astype(jnp.bfloat16) for g in (grad_pre[:, :eighth], grad_pre[:, eighth:])
    )
    up_parts = (up_parts[0], send(up_parts[1], c=1))

    split = (2, NY, half_d // NY, eighth)
    up_sums = chunk_sums(y, *[part.reshape(split) for part in up_parts], True)

    def y_sum(one, three, rest):
        one = send(one, y=1)
        three = send(three, y=3)
        right = send(added(rest[0], three[0]), y=1)
        left = send(added(rest[1], one[0]), y=3)
        return added(rest[2], one[1], left), added(rest[3], three[1], right)

    def z_sum(value):
        got = exchange(value, "z")
        return added(*[got[i] for i in range(nz)])

    def gathered(own, other):
        both = jnp.stack(ordered(fs == 1, own, send(other, fs=1)))
        value = to_all(both, "z").reshape(nz, *both.shape)
        ways = ((y ^ 1, 1), (y ^ 3, 3), (y ^ 2, 2))
        found = [(y, value)] + [(at, send(value, y=flip)) for at, flip in ways]
        near, far = [v for _, v in found[:3]], found[3][1]
        passed = send(jnp.stack(near), c=1)
        places = jnp.stack([at for at, _ in found])
        return (places[:3], near, passed), (places[3:], [far], send(far, c=1)[None])

    d = jnp.concatenate(y_sum(*down_sums)).reshape(nz, rows_down, 2 * half_d)
    d = z_sum(d)
    u = jnp.stack([half.reshape(nz, rows_up, eighth) for half in y_sum(*up_sums)], 1)
    u = z_sum(u)
    near, far = gathered(d[:, :half_d], d[:, half_d:])
    shape = (2, NC, NY, nz * rows_down, half_d)
    grad_down = laid(None, near, c, shape, True, factor)
    grad_down = laid(grad_down, far, c, shape, True, factor)
    near, far = gathered(u[0], u[1])
    grad_up = laid(None, near, c, (half_d, width), False, factor)
    grad_up = laid(grad_up, far, c, (half_d, width), False, factor)

    up_own = fixed(cols_by_core(up_weight, mine))
    up = fixed(jnp.concatenate([up_own, fixed(jnp.concatenate([up_near, up_other], 1))]))
    part = lax.map(lambda r: contract_cols(r, up).astype(jnp.bfloat16), grad_pre.reshape(4, rows // 2, quarter))
    part = part.reshape(2 * rows, 2 * half_d)
    grad_inputs = ring_sum(
        part[:rows, :half_d],
        part[:rows, half_d:],
        part[rows:, :half_d],
        part[rows:, half_d:],
    )
    return grad_inputs, grad_up, grad_down.reshape(width, half_d)


def solution(mesh):
    reps = mesh.shape["rep"]
    split = Mesh(mesh.devices.reshape(reps // (NY * NC), NY, NC, 2, 2), AXES)
    tokens = P((*REP, "tp"), "fs")

    return jax.shard_map(
        per_device,
        mesh=split,
        in_specs=(tokens, P((*REP, "fs"), "tp"), tokens, P("fs", "tp"), P("tp", "fs")),
        out_specs=(tokens, P("fs", "tp"), P("tp", "fs")),
        check_vma=False,
    )
```

```python
import jax
import jax.numpy as jnp
from jax import lax
from jax.experimental import pallas as pl
from jax.experimental.pallas import tpu as pltpu
from jax.sharding import Mesh
from jax.sharding import PartitionSpec as P


NY = 4
NC = 2
AXES = ("z", "y", "c", "fs", "tp")
REP = ("z", "y", "c")


def send(value, y=0, c=0, fs=0, tp=0):
    sizes = [lax.axis_size(axis) for axis in AXES]
    flips = (0, y, c, fs, tp)
    pairs = []
    total = 1
    for size in sizes:
        total *= size
    for source in range(total):
        rest, at = source, []
        for size in reversed(sizes):
            at.append(rest % size)
            rest //= size
        target = 0
        for size, place, flip in zip(sizes, reversed(at), flips):
            target = target * size + (place ^ flip)
        pairs.append((source, target))
    return lax.ppermute(value, AXES, pairs)


def exchange(value, axis):
    return lax.all_to_all(value, axis, 0, 0, tiled=True)


def to_all(value, axis):
    peers = lax.axis_size(axis)
    return exchange(jnp.broadcast_to(value[None], (peers, *value.shape)), axis)


def added(*values):
    total = values[0].astype(jnp.float32)
    for value in values[1:]:
        total = total + value.astype(jnp.float32)
    return total.astype(jnp.bfloat16)


def rows_of(value, start, size):
    return lax.dynamic_slice_in_dim(value, start, size, axis=0)


def cols_of(value, start, size):
    return lax.dynamic_slice_in_dim(value, start, size, axis=1)


def ordered(flag, own, other):
    return jnp.where(flag, other, own), jnp.where(flag, own, other)


def ring_sum(own, near, far, diag):
    return added(own, send(near, fs=1), send(diag, fs=1, tp=1), send(far, tp=1))


def contract_rows(left, right):
    return lax.dot_general(left, right, (((0,), (0,)), ((), ())), preferred_element_type=jnp.float32)


def contract_cols(left, right):
    return lax.dot_general(left, right, (((1,), (1,)), ((), ())), preferred_element_type=jnp.float32)


def tokens_of(own, near, far, diag):
    return jnp.concatenate([jnp.concatenate([own, near], 1), jnp.concatenate([far, diag], 1)], 0)


def laid(out, group, c, shape, by_rows, scale):
    places, own, partner = group
    count, nz, nf, rows, columns = partner.shape
    at = jnp.concatenate([places, c[None]]).astype(jnp.int32)

    def kernel(at, *refs):
        target = refs[-1]

        def put(source, core):
            def step(i, _):
                z, f = i // nf, i % nf
                wide = source[z, f].astype(jnp.float32) * scale
                lines = pl.ds(pl.multiple_of(z * rows, rows), rows)
                if by_rows:
                    target[f, core, 0, lines] = wide
                else:
                    left = pl.multiple_of((f * NC + core) * columns, columns)
                    target[lines, pl.ds(left, columns)] = wide
                return _

            lax.fori_loop(0, nz * nf, step, 0)

        for index in range(count):

            @pl.when(pl.program_id(0) == index)
            def _(source=refs[index]):
                put(source, at[count])

        put(refs[count].at[0], 1 - at[count])

    arguments = (at, *own, partner) + (() if out is None else (out,))
    specs = [pl.BlockSpec((nz, nf, rows, columns), lambda i, at: (0, 0, 0, 0)) for _ in own]
    specs += [pl.BlockSpec((1, nz, nf, rows, columns), lambda i, at: (i, 0, 0, 0, 0))]
    specs += [] if out is None else [pl.BlockSpec(memory_space=pl.ANY)]
    if by_rows:
        out_spec = pl.BlockSpec((nf, NC, 1, nz * rows, columns), lambda i, at: (0, 0, at[i], 0, 0))
    else:
        out_spec = pl.BlockSpec((nz * rows, nf * NC * columns), lambda i, at: (at[i], 0))
    return pl.pallas_call(
        kernel,
        grid_spec=pltpu.PrefetchScalarGridSpec(
            num_scalar_prefetch=1, grid=(count,), in_specs=specs, out_specs=out_spec
        ),
        out_shape=jax.ShapeDtypeStruct(shape, jnp.float32),
        input_output_aliases={} if out is None else {count + 2: 0},
        cost_estimate=pl.CostEstimate(
            flops=2 * partner.size, bytes_accessed=partner.size * 12, transcendentals=0
        ),
    )(*arguments)


def per_device(inputs, pre_act, cotangent, up_weight, down_weight):
    nz = lax.axis_size("z")
    z, y, c, fs, tp = (lax.axis_index(axis) for axis in AXES)
    width = pre_act.shape[1]
    quarter, eighth = width // 2, width // 4
    half_d = inputs.shape[1]
    rows = inputs.shape[0]
    factor = (rows * nz * NY * NC * 2) ** (-0.5)
    mine, theirs = fs * quarter, (1 - fs) * quarter
    first, second = c * eighth, (1 - c) * eighth
    rows_down, rows_up = eighth // (NY * nz), half_d // (NY * nz)
    fixed = lax.optimization_barrier

    def cols_by_core(value, start):
        return jnp.concatenate([cols_of(value, start + first, eighth), cols_of(value, start + second, eighth)], 1)

    down_near = send(rows_of(down_weight, theirs + first + y * (eighth // NY), eighth // NY), fs=1)
    cot_near = send(cotangent, fs=1)
    cot_diag = send(cotangent, fs=1, tp=1)
    pre_near = send(cols_by_core(pre_act, theirs), fs=1)
    down_near = to_all(down_near, "y").reshape(eighth, half_d)
    down_other = send(down_near, c=1)
    cot_far = send(cot_near, fs=1, tp=1)
    in_near = send(inputs, fs=1)
    in_diag = send(inputs, fs=1, tp=1)
    in_far = send(inputs, tp=1)
    up_near = send(cols_by_core(up_weight, theirs), fs=1)

    down_own = fixed(
        jnp.concatenate(
            [rows_of(down_weight, mine + first, eighth), rows_of(down_weight, mine + second, eighth)]
        )
    )
    cot = fixed(tokens_of(cotangent, cot_near, cot_far, cot_diag))
    pre = jnp.concatenate(ordered(fs != tp, cols_by_core(pre_act, mine), pre_near), 0)
    positive = jnp.maximum(pre.astype(jnp.float32), 0.0)
    square = fixed(
        tuple((p * p).astype(jnp.bfloat16) for p in (positive[:, :eighth], positive[:, eighth:]))
    )
    down_part = contract_rows(square[0], cot).astype(jnp.bfloat16)
    down_parts = (down_part, send(contract_rows(square[1], cot).astype(jnp.bfloat16), c=1))

    down_sums = fixed(
        tuple(
            added(*[rows_of(part, (y ^ flip) * (eighth // NY), eighth // NY) for part in down_parts])
            for flip in (1, 3, 2, 0)
        )
    )
    down = fixed(jnp.concatenate([down_own, fixed(jnp.concatenate([down_near, down_other]))], 1))
    grad_pre = fixed((2.0 * positive * contract_cols(cot, down)).astype(jnp.bfloat16))
    grad_pre, *ready = fixed((grad_pre, inputs, in_near, in_far, in_diag, down_sums[3][:1]))[:5]
    x = fixed(tokens_of(*ready))
    up_part = contract_rows(x, grad_pre[:, :eighth]).astype(jnp.bfloat16)
    up_parts = (
        up_part,
        send(contract_rows(x, grad_pre[:, eighth:]).astype(jnp.bfloat16), c=1),
    )
    up_parts = [part.reshape(2, NY * nz * rows_up, eighth) for part in up_parts]
    size = nz * rows_up
    up_sums = fixed(
        tuple(
            added(*[lax.dynamic_slice_in_dim(part, (y ^ flip) * size, size, axis=1) for part in up_parts])
            for flip in (1, 3, 2, 0)
        )
    )

    def y_sum(one, three, two, own):
        got = send(one, y=1), send(three, y=3), send(two, y=2)
        return added(own, *got)

    def z_sum(value):
        got = exchange(value, "z")
        return added(*[got[i] for i in range(nz)])

    def gathered(own, other, cut):
        both = jnp.stack(ordered(fs == 1, own, send(other, fs=1)))
        value = to_all(both, "z").reshape(nz, *both.shape)
        ways = ((y ^ 1, 1), (y ^ 3, 3), (y ^ 2, 2))
        found = [(y, value)] + [(at, send(value, y=flip)) for at, flip in ways]
        places = jnp.stack([at for at, _ in found])
        values = [v for _, v in found]
        near = jnp.stack(values[:3] if cut else values)
        passed = send(near, c=1)
        if not cut:
            return ((places, values, passed),)
        return (places[:3], values[:3], passed), (places[3:], values[3:], send(values[3], c=1)[None])

    d = z_sum(y_sum(*down_sums).reshape(nz, rows_down, 2 * half_d))
    u = y_sum(*up_sums).reshape(2, nz, rows_up, eighth).transpose(1, 0, 2, 3)
    u = z_sum(u)
    (group,) = gathered(d[:, :half_d], d[:, half_d:], False)
    shape = (2, NC, NY, nz * rows_down, half_d)
    grad_down = laid(None, group, c, shape, True, factor)
    near, far = gathered(u[0], u[1], True)
    grad_up = laid(None, near, c, (half_d, width), False, factor)
    grad_up = laid(grad_up, far, c, (half_d, width), False, factor)

    up = fixed(jnp.concatenate([fixed(cols_by_core(up_weight, mine)), up_near]))
    part = contract_cols(grad_pre, up).astype(jnp.bfloat16)
    grad_inputs = ring_sum(
        part[:rows, :half_d],
        part[:rows, half_d:],
        part[rows:, :half_d],
        part[rows:, half_d:],
    )
    return grad_inputs, grad_up, grad_down.reshape(width, half_d)


def solution(mesh):
    reps = mesh.shape["rep"]
    split = Mesh(mesh.devices.reshape(reps // (NY * NC), NY, NC, 2, 2), AXES)
    tokens = P((*REP, "tp"), "fs")

    return jax.shard_map(
        per_device,
        mesh=split,
        in_specs=(tokens, P((*REP, "fs"), "tp"), tokens, P("fs", "tp"), P("tp", "fs")),
        out_specs=(tokens, P("fs", "tp"), P("tp", "fs")),
        check_vma=False,
    )
```
